32 devices in a mesh: gr: 2 (over core), sp: 8 (over z, y), tp: 2 (over x).
Axes of the slice: x: 2, y: 2, z: 4, core: 2. Of those that a mesh axis runs over, the one named last changes fastest.
Arguments:
- tokens: bfloat16 [4, 2048, 2048], P('gr', ('sp', 'tp')), parts along dimension 0, may hold values from -6 to 6
- key_weight: bfloat16 [2048, 1024], P('sp'), may hold values from -0.125 to 0.125
- value_weight: bfloat16 [2048, 1024], P('sp'), may hold values from -0.125 to 0.125
- queries: bfloat16 [4, 1024], P('gr'), parts along dimension 0, may hold values from -6 to 6
- head_offset: float32 [16], replicated, may hold values from -14 to -3.5
- key_bias: bfloat16 [4, 2048, 16], P('gr', ('sp', 'tp')), parts along dimension 0, may hold values from -0.5 to 12.9
Outputs:
- key_cache: bfloat16 [4, 2048, 1024], P('gr', 'sp', 'tp'), parts along dimension 0
- value_cache: bfloat16 [4, 2048, 1024], P('gr', 'sp', 'tp'), parts along dimension 0
- bias_cache: bfloat16 [4, 2048, 16], P('gr', 'sp', 'tp'), parts along dimension 0
- reading: float32 [4, 1024], P('gr', 'tp'), parts along dimension 0
The draws below stay inside these ranges and needn't reach their ends.
There are 2 independent parts, one for each index of `gr`. The reference program is written for one: setup_inputs(seed, part) draws one part's arguments, and reference() takes and returns one part's arrays. A program takes and returns all parts, laid end to end along the dimension named above; an argument that names none is the same for every part. Nothing has to cross between parts.
All inputs are finite; a program needn't handle non-finite values.
Results may differ from the reference program's by a relative error of at most 0.0052.
Values may be sent and summed in bfloat16 or wider, within the bound.
A program may use at most 64 MiB of HBM per device.

```python
import jax
import jax.numpy as jnp
from jax import lax

D = 2048
HEADS = 16
HEAD_DIM = 64
GROUP_SEQUENCES = 2
POS_DEV = 128
PROMPT_LENGTH = 2048


def draw_head_offset(key, part):
    key_a, key_b, key_c, order_key = jax.random.split(jax.random.fold_in(key, 11), 4)
    scale_base = jnp.log(jnp.float32(PROMPT_LENGTH) * 14.6)
    slow_rate = jnp.log(jax.random.uniform(key_a, (HEADS,), jnp.float32, 1.0, 2.3)) - scale_base
    middle_rate = jnp.log(jax.random.uniform(key_c, (HEADS,), jnp.float32, 5.0, 9.0)) - scale_base
    fast_rate = jax.random.uniform(key_b, (HEADS,), jnp.float32, -5.0, -3.5)
    ranks = jax.random.permutation(order_key, HEADS)
    chosen = jnp.where(ranks < HEADS // 2, slow_rate, jnp.where(ranks < 3 * HEADS // 4, middle_rate, fast_rate))
    return chosen.astype(jnp.float32)


def draw_key_bias(key, part):
    key_a, key_b, third_random_key, fourth_random_key = jax.random.split(jax.random.fold_in(key, 23), 4)
    block_count = PROMPT_LENGTH // POS_DEV
    block_tier = jax.random.uniform(key_a, (GROUP_SEQUENCES, block_count, 1, HEADS), jnp.float32, 0.0, 3.4)
    block_tier = jnp.broadcast_to(block_tier, (GROUP_SEQUENCES, block_count, POS_DEV, HEADS)).reshape(GROUP_SEQUENCES, PROMPT_LENGTH, HEADS)
    coarse_portion = jnp.clip(0.25 * jax.random.normal(key_b, (GROUP_SEQUENCES, PROMPT_LENGTH, HEADS), jnp.float32), -0.5, 0.5)
    spike_places = jax.random.randint(third_random_key, (GROUP_SEQUENCES, 3), 0, PROMPT_LENGTH)
    spike_mask = jnp.any(jnp.arange(PROMPT_LENGTH)[None, :, None] == spike_places[:, None, :], axis=-1)
    spike_length = jax.random.uniform(fourth_random_key, (GROUP_SEQUENCES, PROMPT_LENGTH, 1), jnp.float32, 7.5, 9.0)
    grand_sum = block_tier + coarse_portion + jnp.where(spike_mask[:, :, None], spike_length, 0.0)
    return grand_sum.astype(jnp.bfloat16)


def levels(stream_key, shape, shards, smallest, high):
    factor_of = 1.0
    for dim, parts in shards:
        heights = jax.random.uniform(jax.random.fold_in(jax.random.fold_in(stream_key, 6), dim), (parts,), jnp.float32, smallest / len(shards), high / len(shards))
        factor_of = factor_of * jnp.repeat(jnp.exp(heights), shape[dim] // parts).reshape((-1,) + (1,) * (len(shape) - 1 - dim))
    return factor_of


def scatter_about(own_key, dims, scale, reach, pieces=(), kind=jnp.bfloat16):
    result = jax.random.normal(own_key, dims, jnp.float32) * scale
    if len(pieces) > 0:
        result = levels(own_key, dims, pieces, -0.22, 0.18) * result
    return jnp.clip(result, min=-reach, max=reach).astype(kind)


def setup_inputs(seed: int = 0, part: int = 0) -> dict:
    arg_keys = jax.random.split(jax.random.key(seed), 7)
    part_splits = jax.random.split(jax.random.fold_in(arg_keys[6], part), 7)
    return {
        "tokens": scatter_about(part_splits[0], (GROUP_SEQUENCES, PROMPT_LENGTH, D), 1.0, 6.0, ((1, 16),)),
        "key_weight": scatter_about(arg_keys[1], (D, HEADS * HEAD_DIM), D ** -0.5, 0.125, ((0, 8),)),
        "value_weight": scatter_about(arg_keys[2], (D, HEADS * HEAD_DIM), D ** -0.5, 0.125, ((0, 8),)),
        "queries": scatter_about(part_splits[3], (GROUP_SEQUENCES, HEADS * HEAD_DIM), 1.0, 6.0),
        "head_offset": draw_head_offset(jax.random.fold_in(arg_keys[6], 71), part),
        "key_bias": draw_key_bias(jax.random.fold_in(jax.random.fold_in(arg_keys[6], part), 71), part),
    }


def reference(tokens, key_weight, value_weight, queries, head_offset, key_bias):
    score_scale = HEAD_DIM ** (-0.5)

    def one_sequence(inputs):
        tok_rows, key_offsets, query_row = inputs
        key_rows = jnp.dot(tok_rows, key_weight, preferred_element_type=jnp.float32).astype(jnp.bfloat16)
        value_rows = jnp.dot(tok_rows, value_weight, preferred_element_type=jnp.float32).astype(jnp.bfloat16)
        key_heads = key_rows.reshape(PROMPT_LENGTH, HEADS, HEAD_DIM).astype(jnp.float32)
        value_heads = value_rows.reshape(PROMPT_LENGTH, HEADS, HEAD_DIM).astype(jnp.float32)
        query_heads = query_row.reshape(HEADS, HEAD_DIM).astype(jnp.float32)
        logits = jnp.einsum('thc,hc->ht', key_heads, query_heads) * score_scale
        logits = logits + head_offset[:, None] + key_offsets.astype(jnp.float32).T
        fading = jax.nn.log_sigmoid(-logits)
        beyond = lax.cumsum(fading, axis=1, reverse=True) - fading
        weights = jnp.exp(jax.nn.log_sigmoid(logits) + beyond).astype(jnp.bfloat16)
        mixture = jnp.einsum('ht,thc->hc', weights.astype(jnp.float32), value_heads)
        normed = mixture * lax.rsqrt(lax.optimization_barrier(jnp.mean(mixture * mixture, axis=1, keepdims=True)) + 1e-06)
        return (key_rows, value_rows, normed.reshape(HEADS * HEAD_DIM))
    key_rows, value_rows, reading = lax.map(one_sequence, (tokens, key_bias, queries))
    return (key_rows, value_rows, key_bias, reading)
```

```python
import functools

import jax
import jax.numpy as jnp
from jax import lax
from jax.experimental import pallas as pl
from jax.experimental.pallas import tpu as pltpu
from jax.sharding import PartitionSpec as P

MESH = pl.DeviceIdType.MESH
F32 = jnp.float32
BF16 = jnp.bfloat16
SUBS = 2


def ring_place(index, length):
    lane, row = lax.rem(index, 2), index // 2
    return row * (1 - lane) + (length - 1 - row) * lane


def ring_index(place, length):
    lane = place // (length // 2)
    row = place * (1 - lane) + (length - 1 - place) * lane
    return 2 * row + lane


def kernel(
    dims,
    tokens, key_weight, value_weight, queries, head_offset, key_bias,
    key_out, value_out, bias_out, reading_out,
    tok, wts, acc, kv, bias, query, offset, bias_all, packed,
    local_sem, ring_send, ring_recv, pair_send, pair_recv,
    tok_send, tok_recv, bias_send, bias_recv, mix_send, mix_recv, out_sem,
):
    n, tp_count, seqs, pos, width, rows, cols, heads, head_dim, rows_h = dims
    hops = n // 2
    sub_rows = rows // SUBS
    span = tp_count * pos
    me, tp, gr = lax.axis_index("sp"), lax.axis_index("tp"), lax.axis_index("gr")
    place = ring_place(me, n)

    def owner_at(step):
        return ring_index(lax.rem(place + step + n, n), n)

    right, left = owner_at(1), owner_at(-1)
    partner = 1 - gr
    col_start = pl.multiple_of(tp * cols, 128)
    chunked = (width // n) % 128 == 0
    order = [0]
    for h in range(1, hops + 1):
        order.extend([-h, h] if h < hops else [h])
    chunk = width // n if chunked else width
    my_rows = pl.ds(pl.multiple_of(tp * pos, pos), pos)

    weight_copies = [
        pltpu.make_async_copy(
            w.at[:, pl.ds(col_start, cols)], wts.at[part, me], local_sem.at[part]
        )
        for part, w in enumerate((key_weight, value_weight))
    ]
    tok_copy = pltpu.make_async_copy(tokens, tok.at[:, my_rows, :], local_sem.at[2])
    bias_copy = pltpu.make_async_copy(key_bias, bias_all, local_sem.at[3])
    query_copy = pltpu.make_async_copy(queries, query, local_sem.at[4])
    offset_copy = pltpu.make_async_copy(head_offset, offset, local_sem.at[5])
    for c in (*weight_copies, tok_copy, bias_copy, query_copy, offset_copy):
        c.start()

    tp_peers = [lax.rem(tp + k, tp_count) for k in range(1, tp_count)]
    barrier = pltpu.get_barrier_semaphore()
    for target in ({"sp": right}, {"sp": left}, {"gr": partner}, *({"tp": p} for p in tp_peers)):
        pl.semaphore_signal(barrier, inc=1, device_id=target, device_id_type=MESH)

    def ring_copy(direction, hop, sub, step):
        block = wts.at[gr, owner_at(step), pl.ds(sub * sub_rows, sub_rows), :]
        return pltpu.make_async_remote_copy(
            src_ref=block, dst_ref=block,
            send_sem=ring_send.at[direction, hop - 1, sub],
            recv_sem=ring_recv.at[direction, hop - 1, sub],
            device_id={"sp": right if direction == 0 else left}, device_id_type=MESH,
        )

    def step_of(direction, hop):
        return -hop if direction == 0 else hop

    def sent(direction, hop, sub):
        return ring_copy(direction, hop, sub, step_of(direction, hop - 1))

    def got(direction, hop, sub):
        return ring_copy(direction, hop, sub, step_of(direction, hop))

    def used(direction, hop, sub):
        return hop < hops or (hop == hops and sub % 2 == direction)

    def pair_copy(direction, hop, sub, part):
        block = wts.at[part, owner_at(step_of(direction, hop)), pl.ds(sub * sub_rows, sub_rows), :]
        return pltpu.make_async_remote_copy(
            src_ref=block, dst_ref=block,
            send_sem=pair_send.at[direction, hop - 1, sub],
            recv_sem=pair_recv.at[direction, hop - 1, sub],
            device_id={"gr": partner}, device_id_type=MESH,
        )

    def tok_columns(i):
        if not chunked:
            return pl.ds(0, width)
        return pl.ds(pl.multiple_of(owner_at(order[i]) * chunk, 128), chunk)

    chunk_count = len(order) if chunked else 1

    def tok_move(i, k, source):
        place_rows = pl.ds(pl.multiple_of(source * pos, pos), pos)
        block = tok.at[:, place_rows, tok_columns(i)]
        return pltpu.make_async_remote_copy(
            src_ref=block, dst_ref=block,
            send_sem=tok_send.at[i, k], recv_sem=tok_recv.at[i, k],
            device_id={"tp": lax.rem(tp + k + 1, tp_count)}, device_id_type=MESH,
        )

    def bias_move(k, source, target):
        return pltpu.make_async_remote_copy(
            src_ref=bias_all.at[:, target], dst_ref=bias.at[source],
            send_sem=bias_send.at[k], recv_sem=bias_recv.at[k],
            device_id={"tp": lax.rem(tp + k + 1, tp_count)}, device_id_type=MESH,
        )

    pl.semaphore_wait(barrier, 3 + len(tp_peers))
    for c in weight_copies:
        c.wait()
    sent_list = []

    def launch(c):
        c.start()
        sent_list.append(c)

    for sub in range(SUBS):
        for direction in range(2):
            if used(direction, 1, sub):
                launch(sent(direction, 1, sub))
    tok_copy.wait()
    for i in range(chunk_count):
        for k in range(tp_count - 1):
            launch(tok_move(i, k, tp))
    bias_copy.wait()
    for k in range(tp_count - 1):
        launch(bias_move(k, tp, lax.rem(tp + k + 1, tp_count)))
    query_copy.wait()
    offset_copy.wait()

    def tokens_ready(i):
        for k in range(tp_count - 1):
            tok_move(i, k, lax.rem(tp + tp_count - k - 1, tp_count)).wait_recv()

    def multiply(i, last):
        owner = owner_at(order[i])
        for part in range(2):
            w = wts[part, owner]

            def body(s, carry):
                x = tok[s, :, tok_columns(i)]
                y = jnp.dot(x, w, preferred_element_type=F32)
                if i > 0:
                    y = acc[part, s] + y
                if last:
                    kv[part, s] = y.astype(BF16)
                else:
                    acc[part, s] = y
                return carry

            lax.fori_loop(0, seqs, body, 0)
            if last:
                pltpu.make_async_copy(
                    kv.at[part], (key_out, value_out)[part], out_sem.at[part]
                ).start()

    def pair_ready(hop):
        for direction in range(2):
            for sub in range(SUBS):
                if used(direction, hop, sub):
                    pair_copy(direction, hop, sub, partner).wait_recv()

    def steps_of_hop(hop):
        if hop == 0:
            return [0]
        first = 1 + 2 * (hop - 1)
        return [first, first + 1] if hop < hops else [first]

    def compute_hop(hop):
        if hop > 0:
            pair_ready(hop)
        if chunked:
            for i in steps_of_hop(hop):
                tokens_ready(i)
                multiply(i, i == len(order) - 1)

    for hop in range(1, hops + 1):
        for sub in range(SUBS):
            for direction in range(2):
                if not used(direction, hop, sub):
                    continue
                got(direction, hop, sub).wait_recv()
                if hop < hops and used(direction, hop + 1, sub):
                    launch(sent(direction, hop + 1, sub))
                launch(pair_copy(direction, hop, sub, gr))
        compute_hop(hop - 1)
    compute_hop(hops)

    if not chunked:
        tokens_ready(0)
        tile = pos
        for part in range(2):
            w = wts[part].reshape(width, cols)

            def body(j, carry):
                s, r = j // (span // tile), lax.rem(j, span // tile)
                where = pl.ds(pl.multiple_of(r * tile, tile), tile)
                y = jnp.dot(tok[s, where, :], w, preferred_element_type=F32)
                kv[part, s, where, :] = y.astype(BF16)
                return carry

            lax.fori_loop(0, seqs * (span // tile), body, 0)
            pltpu.make_async_copy(
                kv.at[part], (key_out, value_out)[part], out_sem.at[part]
            ).start()

    for k in range(tp_count - 1):
        bias_move(k, lax.rem(tp + tp_count - k - 1, tp_count), tp).wait_recv()
    bias[tp] = bias_all[:, tp]

    row_id = lax.broadcasted_iota(jnp.int32, (rows_h, cols), 0)
    col_id = lax.broadcasted_iota(jnp.int32, (rows_h, cols), 1)
    own = row_id == col_id // head_dim
    q = query[:, pl.ds(col_start, cols)].astype(F32)
    total_heads = offset.shape[1]
    pick = lax.broadcasted_iota(jnp.int32, (rows_h, total_heads), 1) == (
        lax.broadcasted_iota(jnp.int32, (rows_h, total_heads), 0) + tp * heads
    )
    offset_col = jnp.sum(jnp.where(pick, offset[...], 0.0), axis=1, keepdims=True)
    logits = []
    for s in range(seqs):
        q_rows = jnp.where(own, q[s : s + 1], 0.0).astype(BF16)
        b = jnp.concatenate([bias[t, s] for t in range(tp_count)], axis=1)
        bias_out[s] = b
        b = b.astype(F32)
        if rows_h > heads:
            b = jnp.concatenate([b, jnp.zeros((rows_h - heads, span), F32)], axis=0)
        logits.append(
            lax.dot_general(
                q_rows, kv[0, s], (((1,), (1,)), ((), ())), preferred_element_type=F32
            )
            * (head_dim**-0.5)
            + offset_col
            + b
        )
    logits = jnp.concatenate(logits, axis=0)
    soft = jnp.log1p(jnp.exp(-jnp.abs(logits)))
    fading = -jnp.maximum(logits, 0.0) - soft
    taking = jnp.minimum(logits, 0.0) - soft
    high = fading.astype(BF16)
    rest = fading - high.astype(F32)
    mid = rest.astype(BF16)
    low = (rest - mid.astype(F32)).astype(BF16)
    later = (
        lax.broadcasted_iota(jnp.int32, (span, span), 0)
        > lax.broadcasted_iota(jnp.int32, (span, span), 1)
    ).astype(F32).astype(BF16)
    sums = jnp.dot(
        jnp.concatenate([high, mid, low], axis=0), later, preferred_element_type=F32
    )
    m = seqs * rows_h
    within = sums[:m] + sums[m : 2 * m] + sums[2 * m :]
    weights = jnp.exp(taking + within).astype(BF16)
    totals = jnp.sum(fading, axis=1, keepdims=True)
    for s in range(seqs):
        at = slice(s * rows_h, (s + 1) * rows_h)
        partial = jnp.dot(weights[at], kv[1, s], preferred_element_type=F32)
        packed[me, s : s + 1] = jnp.sum(jnp.where(own, partial, 0.0), axis=0, keepdims=True)
        packed[me, seqs + s : seqs + s + 1] = jnp.sum(
            jnp.where(own, totals[at], 0.0), axis=0, keepdims=True
        )

    def mix_move(k, source):
        return pltpu.make_async_remote_copy(
            src_ref=packed.at[source], dst_ref=packed.at[source],
            send_sem=mix_send.at[k - 1], recv_sem=mix_recv.at[k - 1],
            device_id={"sp": lax.rem(me + k, n)}, device_id_type=MESH,
        )

    for k in range(1, n):
        launch(mix_move(k, me))
    for k in range(1, n):
        mix_move(k, lax.rem(me + n - k, n)).wait_recv()
    mixture = jnp.zeros((seqs, cols), F32)
    carry = jnp.zeros((seqs, cols), F32)
    for at in range(n - 1, -1, -1):
        mixture = mixture + jnp.exp(carry) * packed[at, :seqs]
        carry = carry + packed[at, seqs:]
    for s in range(seqs):
        x = mixture[s : s + 1]
        mean = jnp.sum(jnp.where(own, x * x, 0.0), axis=1, keepdims=True) / head_dim
        scale = jnp.sum(jnp.where(own, lax.rsqrt(mean + 1e-06), 0.0), axis=0, keepdims=True)
        reading_out[s : s + 1] = x * scale

    for c in sent_list:
        c.wait_send()
    for part in range(2):
        pltpu.make_async_copy(
            kv.at[part], (key_out, value_out)[part], out_sem.at[part]
        ).wait()


def per_device(tokens, key_weight, value_weight, queries, head_offset, key_bias):
    n, tp_count = lax.axis_size("sp"), lax.axis_size("tp")
    assert n % 2 == 0 and lax.axis_size("gr") == 2
    seqs, pos, width = tokens.shape
    rows, kv_width = key_weight.shape
    head_count = head_offset.shape[0]
    head_dim = kv_width // head_count
    cols = kv_width // tp_count
    heads = head_count // tp_count
    rows_h = max(8, heads)
    span = tp_count * pos
    hops = n // 2
    bias_rows = jnp.transpose(key_bias, (0, 2, 1)).reshape(seqs, tp_count, heads, pos)
    dims = (n, tp_count, seqs, pos, width, rows, cols, heads, head_dim, rows_h)
    peers = max(tp_count - 1, 1)
    chunks = n if (width // n) % 128 == 0 else 1
    dma = pltpu.SemaphoreType.DMA
    key_cache, value_cache, bias_cache, reading = pl.pallas_call(
        functools.partial(kernel, dims),
        out_shape=(
            jax.ShapeDtypeStruct((seqs, span, cols), BF16),
            jax.ShapeDtypeStruct((seqs, span, cols), BF16),
            jax.ShapeDtypeStruct((seqs, heads, span), BF16),
            jax.ShapeDtypeStruct((seqs, cols), F32),
        ),
        in_specs=[pl.BlockSpec(memory_space=pl.ANY)] * 6,
        out_specs=[
            pl.BlockSpec(memory_space=pl.ANY),
            pl.BlockSpec(memory_space=pl.ANY),
            pl.BlockSpec(memory_space=pltpu.VMEM),
            pl.BlockSpec(memory_space=pltpu.VMEM),
        ],
        scratch_shapes=[
            pltpu.VMEM((seqs, span, width), BF16),
            pltpu.VMEM((2, n, rows, cols), BF16),
            pltpu.VMEM((2, seqs, span, cols), F32),
            pltpu.VMEM((2, seqs, span, cols), BF16),
            pltpu.VMEM((tp_count, seqs, heads, pos), BF16),
            pltpu.VMEM(queries.shape, BF16),
            pltpu.VMEM((1, head_count), F32),
            pltpu.VMEM((seqs, tp_count, heads, pos), BF16),
            pltpu.VMEM((n, 2 * seqs, cols), F32),
            dma((6,)),
            dma((2, hops, SUBS)),
            dma((2, hops, SUBS)),
            dma((2, hops, SUBS)),
            dma((2, hops, SUBS)),
            dma((chunks, peers)),
            dma((chunks, peers)),
            dma((peers,)),
            dma((peers,)),
            dma((n - 1,)),
            dma((n - 1,)),
            dma((2,)),
        ],
        compiler_params=pltpu.CompilerParams(collective_id=0, has_side_effects=True),
        name="prefill_read",
    )(tokens, key_weight, value_weight, queries, head_offset.reshape(1, head_count), bias_rows)
    return key_cache, value_cache, jnp.transpose(bias_cache, (0, 2, 1)), reading


def solution(mesh):
    in_specs = (
        P("gr", ("sp", "tp"), None),
        P("sp", None),
        P("sp", None),
        P("gr", None),
        P(),
        P("gr", ("sp", "tp"), None),
    )
    out_specs = (P("gr", "sp", "tp"), P("gr", "sp", "tp"), P("gr", "sp", "tp"), P("gr", "tp"))
    return jax.shard_map(
        per_device, mesh=mesh, in_specs=in_specs, out_specs=out_specs, check_vma=False
    )
```

```python
import functools

import jax
import jax.numpy as jnp
from jax import lax
from jax.experimental import pallas as pl
from jax.experimental.pallas import tpu as pltpu
from jax.sharding import PartitionSpec as P

MESH = pl.DeviceIdType.MESH
F32 = jnp.float32
BF16 = jnp.bfloat16
SUBS = 2


def ring_place(index, length):
    lane, row = lax.rem(index, 2), index // 2
    return row * (1 - lane) + (length - 1 - row) * lane


def ring_index(place, length):
    lane = place // (length // 2)
    row = place * (1 - lane) + (length - 1 - place) * lane
    return 2 * row + lane


def kernel(
    dims,
    tokens, key_weight, value_weight, queries, head_offset, key_bias,
    kv, bias_out, packed,
    tok, wts, acc, bias, query, offset, bias_all,
    local_sem, ring_send, ring_recv, pair_send, pair_recv,
    tok_send, tok_recv, bias_send, bias_recv, mix_send, mix_recv,
):
    n, tp_count, seqs, pos, width, rows, cols, heads, head_dim, rows_h = dims
    hops = n // 2
    sub_rows = rows // SUBS
    span = tp_count * pos
    me, tp, gr = lax.axis_index("sp"), lax.axis_index("tp"), lax.axis_index("gr")
    place = ring_place(me, n)

    def owner_at(step):
        return ring_index(lax.rem(place + step + n, n), n)

    right, left = owner_at(1), owner_at(-1)
    partner = 1 - gr
    col_start = pl.multiple_of(tp * cols, 128)
    chunked = (width // n) % 128 == 0
    order = [0]
    for h in range(1, hops + 1):
        order.extend([-h, h] if h < hops else [h])
    chunk = width // n if chunked else width
    my_rows = pl.ds(pl.multiple_of(tp * pos, pos), pos)

    weight_copies = [
        pltpu.make_async_copy(
            w.at[:, pl.ds(col_start, cols)], wts.at[part, me], local_sem.at[part]
        )
        for part, w in enumerate((key_weight, value_weight))
    ]
    tok_copy = pltpu.make_async_copy(tokens, tok.at[:, my_rows, :], local_sem.at[2])
    bias_copy = pltpu.make_async_copy(key_bias, bias_all, local_sem.at[3])
    query_copy = pltpu.make_async_copy(queries, query, local_sem.at[4])
    offset_copy = pltpu.make_async_copy(head_offset, offset, local_sem.at[5])
    for c in (*weight_copies, tok_copy, bias_copy, query_copy, offset_copy):
        c.start()

    tp_peers = [lax.rem(tp + k, tp_count) for k in range(1, tp_count)]
    barrier = pltpu.get_barrier_semaphore()
    for target in ({"sp": right}, {"sp": left}, {"gr": partner}, *({"tp": p} for p in tp_peers)):
        pl.semaphore_signal(barrier, inc=1, device_id=target, device_id_type=MESH)

    def ring_copy(direction, hop, sub, step):
        block = wts.at[gr, owner_at(step), pl.ds(sub * sub_rows, sub_rows), :]
        return pltpu.make_async_remote_copy(
            src_ref=block, dst_ref=block,
            send_sem=ring_send.at[direction, hop - 1, sub],
            recv_sem=ring_recv.at[direction, hop - 1, sub],
            device_id={"sp": right if direction == 0 else left}, device_id_type=MESH,
        )

    def step_of(direction, hop):
        return -hop if direction == 0 else hop

    def sent(direction, hop, sub):
        return ring_copy(direction, hop, sub, step_of(direction, hop - 1))

    def got(direction, hop, sub):
        return ring_copy(direction, hop, sub, step_of(direction, hop))

    def used(direction, hop, sub):
        return hop < hops or (hop == hops and sub % 2 == direction)

    def pair_copy(direction, hop, sub, part):
        block = wts.at[part, owner_at(step_of(direction, hop)), pl.ds(sub * sub_rows, sub_rows), :]
        return pltpu.make_async_remote_copy(
            src_ref=block, dst_ref=block,
            send_sem=pair_send.at[direction, hop - 1, sub],
            recv_sem=pair_recv.at[direction, hop - 1, sub],
            device_id={"gr": partner}, device_id_type=MESH,
        )

    def tok_columns(i):
        if not chunked:
            return pl.ds(0, width)
        return pl.ds(pl.multiple_of(owner_at(order[i]) * chunk, 128), chunk)

    chunk_count = len(order) if chunked else 1

    def tok_move(i, k, source):
        place_rows = pl.ds(pl.multiple_of(source * pos, pos), pos)
        block = tok.at[:, place_rows, tok_columns(i)]
        return pltpu.make_async_remote_copy(
            src_ref=block, dst_ref=block,
            send_sem=tok_send.at[i, k], recv_sem=tok_recv.at[i, k],
            device_id={"tp": lax.rem(tp + k + 1, tp_count)}, device_id_type=MESH,
        )

    def bias_move(k, source, target):
        return pltpu.make_async_remote_copy(
            src_ref=bias_all.at[:, target], dst_ref=bias.at[source],
            send_sem=bias_send.at[k], recv_sem=bias_recv.at[k],
            device_id={"tp": lax.rem(tp + k + 1, tp_count)}, device_id_type=MESH,
        )

    pl.semaphore_wait(barrier, 3 + len(tp_peers))
    for c in weight_copies:
        c.wait()
    sent_list = []

    def launch(c):
        c.start()
        sent_list.append(c)

    for sub in range(SUBS):
        for direction in range(2):
            if used(direction, 1, sub):
                launch(sent(direction, 1, sub))
    tok_copy.wait()
    for i in range(chunk_count):
        for k in range(tp_count - 1):
            launch(tok_move(i, k, tp))
    bias_copy.wait()
    for k in range(tp_count - 1):
        launch(bias_move(k, tp, lax.rem(tp + k + 1, tp_count)))
    query_copy.wait()
    offset_copy.wait()

    def tokens_ready(i):
        for k in range(tp_count - 1):
            tok_move(i, k, lax.rem(tp + tp_count - k - 1, tp_count)).wait_recv()

    def multiply(i, last):
        owner = owner_at(order[i])
        for part in range(2):
            w = wts[part, owner]

            def body(s, carry):
                x = tok[s, :, tok_columns(i)]
                y = jnp.dot(x, w, preferred_element_type=F32)
                if i > 0:
                    y = acc[part, s] + y
                if last:
                    kv[part, s] = y.astype(BF16)
                else:
                    acc[part, s] = y
                return carry

            lax.fori_loop(0, seqs, body, 0)

    def pair_ready(hop):
        for direction in range(2):
            for sub in range(SUBS):
                if used(direction, hop, sub):
                    pair_copy(direction, hop, sub, partner).wait_recv()

    def steps_of_hop(hop):
        if hop == 0:
            return [0]
        first = 1 + 2 * (hop - 1)
        return [first, first + 1] if hop < hops else [first]

    def compute_hop(hop):
        if hop > 0:
            pair_ready(hop)
        if chunked:
            for i in steps_of_hop(hop):
                tokens_ready(i)
                multiply(i, i == len(order) - 1)

    for hop in range(1, hops + 1):
        for sub in range(SUBS):
            for direction in range(2):
                if not used(direction, hop, sub):
                    continue
                got(direction, hop, sub).wait_recv()
                if hop < hops and used(direction, hop + 1, sub):
                    launch(sent(direction, hop + 1, sub))
                launch(pair_copy(direction, hop, sub, gr))
        compute_hop(hop - 1)
    compute_hop(hops)

    if not chunked:
        tokens_ready(0)
        tile = pos
        for part in range(2):
            w = wts[part].reshape(width, cols)

            def body(j, carry):
                s, r = j // (span // tile), lax.rem(j, span // tile)
                where = pl.ds(pl.multiple_of(r * tile, tile), tile)
                y = jnp.dot(tok[s, where, :], w, preferred_element_type=F32)
                kv[part, s, where, :] = y.astype(BF16)
                return carry

            lax.fori_loop(0, seqs * (span // tile), body, 0)

    for k in range(tp_count - 1):
        bias_move(k, lax.rem(tp + tp_count - k - 1, tp_count), tp).wait_recv()
    bias[tp] = bias_all[:, tp]

    row_id = lax.broadcasted_iota(jnp.int32, (rows_h, cols), 0)
    col_id = lax.broadcasted_iota(jnp.int32, (rows_h, cols), 1)
    own = row_id == col_id // head_dim
    q = query[:, pl.ds(col_start, cols)].astype(F32)
    total_heads = offset.shape[1]
    pick = lax.broadcasted_iota(jnp.int32, (rows_h, total_heads), 1) == (
        lax.broadcasted_iota(jnp.int32, (rows_h, total_heads), 0) + tp * heads
    )
    offset_col = jnp.sum(jnp.where(pick, offset[...], 0.0), axis=1, keepdims=True)
    logits = []
    for s in range(seqs):
        q_rows = jnp.where(own, q[s : s + 1], 0.0).astype(BF16)
        b = jnp.concatenate([bias[t, s] for t in range(tp_count)], axis=1)
        bias_out[s] = b
        b = b.astype(F32)
        if rows_h > heads:
            b = jnp.concatenate([b, jnp.zeros((rows_h - heads, span), F32)], axis=0)
        logits.append(
            lax.dot_general(
                q_rows, kv[0, s], (((1,), (1,)), ((), ())), preferred_element_type=F32
            )
            * (head_dim**-0.5)
            + offset_col
            + b
        )
    logits = jnp.concatenate(logits, axis=0)
    soft = jnp.log1p(jnp.exp(-jnp.abs(logits)))
    fading = -jnp.maximum(logits, 0.0) - soft
    taking = jnp.minimum(logits, 0.0) - soft
    high = fading.astype(BF16)
    rest = fading - high.astype(F32)
    mid = rest.astype(BF16)
    low = (rest - mid.astype(F32)).astype(BF16)
    later = (
        lax.broadcasted_iota(jnp.int32, (span, span), 0)
        > lax.broadcasted_iota(jnp.int32, (span, span), 1)
    ).astype(F32).astype(BF16)
    sums = jnp.dot(
        jnp.concatenate([high, mid, low], axis=0), later, preferred_element_type=F32
    )
    m = seqs * rows_h
    within = sums[:m] + sums[m : 2 * m] + sums[2 * m :]
    weights = jnp.exp(taking + within).astype(BF16)
    totals = jnp.sum(fading, axis=1, keepdims=True)
    for s in range(seqs):
        at = slice(s * rows_h, (s + 1) * rows_h)
        partial = jnp.dot(weights[at], kv[1, s], preferred_element_type=F32)
        packed[me, s : s + 1] = jnp.sum(jnp.where(own, partial, 0.0), axis=0, keepdims=True)
        packed[me, seqs + s : seqs + s + 1] = jnp.sum(
            jnp.where(own, totals[at], 0.0), axis=0, keepdims=True
        )

    def mix_move(k, source):
        return pltpu.make_async_remote_copy(
            src_ref=packed.at[source], dst_ref=packed.at[source],
            send_sem=mix_send.at[k - 1], recv_sem=mix_recv.at[k - 1],
            device_id={"sp": lax.rem(me + k, n)}, device_id_type=MESH,
        )

    for k in range(1, n):
        launch(mix_move(k, me))
    for k in range(1, n):
        mix_move(k, lax.rem(me + n - k, n)).wait_recv()
    for c in sent_list:
        c.wait_send()


def finish(n, head_dim, kv, bias, packed, key_out, value_out, bias_out, reading_out, sems):
    moves = [
        pltpu.make_async_copy(kv.at[0], key_out, sems.at[0]),
        pltpu.make_async_copy(kv.at[1], value_out, sems.at[1]),
        pltpu.make_async_copy(bias, bias_out, sems.at[2]),
    ]
    for c in moves:
        c.start()
    seqs, cols = reading_out.shape
    rows_h = max(8, cols // head_dim)
    row_id = lax.broadcasted_iota(jnp.int32, (rows_h, cols), 0)
    col_id = lax.broadcasted_iota(jnp.int32, (rows_h, cols), 1)
    own = row_id == col_id // head_dim
    mixture = jnp.zeros((seqs, cols), F32)
    carry = jnp.zeros((seqs, cols), F32)
    for at in range(n - 1, -1, -1):
        mixture = mixture + jnp.exp(carry) * packed[at, :seqs]
        carry = carry + packed[at, seqs:]
    for s in range(seqs):
        x = mixture[s : s + 1]
        mean = jnp.sum(jnp.where(own, x * x, 0.0), axis=1, keepdims=True) / head_dim
        scale = jnp.sum(jnp.where(own, lax.rsqrt(mean + 1e-06), 0.0), axis=0, keepdims=True)
        reading_out[s : s + 1] = x * scale
    for c in moves:
        c.wait()


def per_device(tokens, key_weight, value_weight, queries, head_offset, key_bias):
    n, tp_count = lax.axis_size("sp"), lax.axis_size("tp")
    assert n % 2 == 0 and lax.axis_size("gr") == 2
    seqs, pos, width = tokens.shape
    rows, kv_width = key_weight.shape
    head_count = head_offset.shape[0]
    head_dim = kv_width // head_count
    cols = kv_width // tp_count
    heads = head_count // tp_count
    rows_h = max(8, heads)
    span = tp_count * pos
    hops = n // 2
    bias_rows = jnp.transpose(key_bias, (0, 2, 1)).reshape(seqs, tp_count, heads, pos)
    dims = (n, tp_count, seqs, pos, width, rows, cols, heads, head_dim, rows_h)
    peers = max(tp_count - 1, 1)
    chunks = n if (width // n) % 128 == 0 else 1
    dma = pltpu.SemaphoreType.DMA
    kv, bias_held, packed = pl.pallas_call(
        functools.partial(kernel, dims),
        out_shape=(
            jax.ShapeDtypeStruct((2, seqs, span, cols), BF16),
            jax.ShapeDtypeStruct((seqs, heads, span), BF16),
            jax.ShapeDtypeStruct((n, 2 * seqs, cols), F32),
        ),
        in_specs=[pl.BlockSpec(memory_space=pltpu.HBM)] * 6,
        out_specs=[pl.BlockSpec(memory_space=pltpu.VMEM)] * 3,
        scratch_shapes=[
            pltpu.VMEM((seqs, span, width), BF16),
            pltpu.VMEM((2, n, rows, cols), BF16),
            pltpu.VMEM((2, seqs, span, cols), F32),
            pltpu.VMEM((tp_count, seqs, heads, pos), BF16),
            pltpu.VMEM(queries.shape, BF16),
            pltpu.VMEM((1, head_count), F32),
            pltpu.VMEM((seqs, tp_count, heads, pos), BF16),
            dma((6,)),
            dma((2, hops, SUBS)),
            dma((2, hops, SUBS)),
            dma((2, hops, SUBS)),
            dma((2, hops, SUBS)),
            dma((chunks, peers)),
            dma((chunks, peers)),
            dma((peers,)),
            dma((peers,)),
            dma((n - 1,)),
            dma((n - 1,)),
        ],
        compiler_params=pltpu.CompilerParams(
            collective_id=0, has_side_effects=True, vmem_limit_bytes=36 * 2**20
        ),
        name="prefill",
    )(*(pltpu.with_memory_space_constraint(a, pltpu.HBM) for a in (tokens, key_weight, value_weight, queries, head_offset.reshape(1, head_count), bias_rows)))
    key_cache, value_cache, bias_cache, reading = pl.pallas_call(
        functools.partial(finish, n, head_dim),
        out_shape=(
            jax.ShapeDtypeStruct((seqs, span, cols), BF16),
            jax.ShapeDtypeStruct((seqs, span, cols), BF16),
            jax.ShapeDtypeStruct((seqs, heads, span), BF16),
            jax.ShapeDtypeStruct((seqs, cols), F32),
        ),
        in_specs=[
            pl.BlockSpec(memory_space=pl.ANY),
            pl.BlockSpec(memory_space=pl.ANY),
            pl.BlockSpec(memory_space=pltpu.VMEM),
        ],
        out_specs=[
            pl.BlockSpec(memory_space=pl.ANY),
            pl.BlockSpec(memory_space=pl.ANY),
            pl.BlockSpec(memory_space=pl.ANY),
            pl.BlockSpec(memory_space=pltpu.VMEM),
        ],
        scratch_shapes=[dma((3,))],
        compiler_params=pltpu.CompilerParams(vmem_limit_bytes=4 * 2**20),
        name="finish",
    )(kv, bias_held, packed)
    return key_cache, value_cache, jnp.transpose(bias_cache, (0, 2, 1)), reading


def solution(mesh):
    in_specs = (
        P("gr", ("sp", "tp"), None),
        P("sp", None),
        P("sp", None),
        P("gr", None),
        P(),
        P("gr", ("sp", "tp"), None),
    )
    out_specs = (P("gr", "sp", "tp"), P("gr", "sp", "tp"), P("gr", "sp", "tp"), P("gr", "tp"))
    return jax.shard_map(
        per_device, mesh=mesh, in_specs=in_specs, out_specs=out_specs, check_vma=False
    )
```

```python
import functools

import jax
import jax.numpy as jnp
from jax import lax
from jax.experimental import pallas as pl
from jax.experimental.pallas import tpu as pltpu
from jax.sharding import PartitionSpec as P

MESH = pl.DeviceIdType.MESH
F32 = jnp.float32
BF16 = jnp.bfloat16
SUBS = 4


def ring_place(index, length):
    lane, row = lax.rem(index, 2), index // 2
    return row * (1 - lane) + (length - 1 - row) * lane


def ring_index(place, length):
    lane = place // (length // 2)
    row = place * (1 - lane) + (length - 1 - place) * lane
    return 2 * row + lane


def kernel(
    dims,
    tokens, key_weight, value_weight, queries, head_offset, key_bias,
    kv, bias_out, packed,
    tok, wts, acc, bias, query, offset, bias_all,
    local_sem, ring_send, ring_recv, pair_send, pair_recv,
    tok_send, tok_recv, bias_send, bias_recv, mix_send, mix_recv,
):
    n, tp_count, seqs, pos, width, rows, cols, heads, head_dim, rows_h = dims
    hops = n // 2
    sub_rows = rows // SUBS
    span = tp_count * pos
    me, tp, gr = lax.axis_index("sp"), lax.axis_index("tp"), lax.axis_index("gr")
    place = ring_place(me, n)

    def owner_at(step):
        return ring_index(lax.rem(place + step + n, n), n)

    right, left = owner_at(1), owner_at(-1)
    partner = 1 - gr
    col_start = pl.multiple_of(tp * cols, 128)
    chunked = (width // n) % 128 == 0
    order = [0]
    for h in range(1, hops + 1):
        order.extend([-h, h] if h < hops else [h])
    chunk = width // n if chunked else width
    my_rows = pl.ds(pl.multiple_of(tp * pos, pos), pos)

    weight_copies = [
        pltpu.make_async_copy(
            w.at[:, pl.ds(col_start, cols)], wts.at[part, me], local_sem.at[part]
        )
        for part, w in enumerate((key_weight, value_weight))
    ]
    tok_copy = pltpu.make_async_copy(tokens, tok.at[:, my_rows, :], local_sem.at[2])
    bias_copy = pltpu.make_async_copy(key_bias, bias_all, local_sem.at[3])
    query_copy = pltpu.make_async_copy(queries, query, local_sem.at[4])
    offset_copy = pltpu.make_async_copy(head_offset, offset, local_sem.at[5])
    for c in (*weight_copies, tok_copy, bias_copy, query_copy, offset_copy):
        c.start()

    tp_peers = [lax.rem(tp + k, tp_count) for k in range(1, tp_count)]
    barrier = pltpu.get_barrier_semaphore()
    for target in ({"sp": right}, {"sp": left}, {"gr": partner}, *({"tp": p} for p in tp_peers)):
        pl.semaphore_signal(barrier, inc=1, device_id=target, device_id_type=MESH)

    def ring_copy(direction, hop, sub, step):
        block = wts.at[gr, owner_at(step), pl.ds(sub * sub_rows, sub_rows), :]
        return pltpu.make_async_remote_copy(
            src_ref=block, dst_ref=block,
            send_sem=ring_send.at[direction, hop - 1, sub],
            recv_sem=ring_recv.at[direction, hop - 1, sub],
            device_id={"sp": right if direction == 0 else left}, device_id_type=MESH,
        )

    def step_of(direction, hop):
        return -hop if direction == 0 else hop

    def sent(direction, hop, sub):
        return ring_copy(direction, hop, sub, step_of(direction, hop - 1))

    def got(direction, hop, sub):
        return ring_copy(direction, hop, sub, step_of(direction, hop))

    def used(direction, hop, sub):
        return hop < hops or (hop == hops and sub % 2 == direction)

    def pair_copy(direction, hop, sub, part):
        block = wts.at[part, owner_at(step_of(direction, hop)), pl.ds(sub * sub_rows, sub_rows), :]
        return pltpu.make_async_remote_copy(
            src_ref=block, dst_ref=block,
            send_sem=pair_send.at[direction, hop - 1, sub],
            recv_sem=pair_recv.at[direction, hop - 1, sub],
            device_id={"gr": partner}, device_id_type=MESH,
        )

    def tok_columns(i):
        if not chunked:
            return pl.ds(0, width)
        return pl.ds(pl.multiple_of(owner_at(order[i]) * chunk, 128), chunk)

    chunk_count = len(order) if chunked else 1

    def tok_move(i, k, source):
        place_rows = pl.ds(pl.multiple_of(source * pos, pos), pos)
        block = tok.at[:, place_rows, tok_columns(i)]
        return pltpu.make_async_remote_copy(
            src_ref=block, dst_ref=block,
            send_sem=tok_send.at[i, k], recv_sem=tok_recv.at[i, k],
            device_id={"tp": lax.rem(tp + k + 1, tp_count)}, device_id_type=MESH,
        )

    def bias_move(k, source, target):
        return pltpu.make_async_remote_copy(
            src_ref=bias_all.at[:, target], dst_ref=bias.at[source],
            send_sem=bias_send.at[k], recv_sem=bias_recv.at[k],
            device_id={"tp": lax.rem(tp + k + 1, tp_count)}, device_id_type=MESH,
        )

    pl.semaphore_wait(barrier, 3 + len(tp_peers))
    for c in weight_copies:
        c.wait()
    sent_list = []

    def launch(c):
        c.start()
        sent_list.append(c)

    for sub in range(SUBS):
        for direction in range(2):
            if used(direction, 1, sub):
                launch(sent(direction, 1, sub))
    tok_copy.wait()
    for i in range(chunk_count):
        for k in range(tp_count - 1):
            launch(tok_move(i, k, tp))
    bias_copy.wait()
    for k in range(tp_count - 1):
        launch(bias_move(k, tp, lax.rem(tp + k + 1, tp_count)))
    query_copy.wait()
    offset_copy.wait()

    def tokens_ready(i):
        for k in range(tp_count - 1):
            tok_move(i, k, lax.rem(tp + tp_count - k - 1, tp_count)).wait_recv()

    def multiply(i):
        owner = owner_at(order[i])
        for part in range(2):
            w = wts[part, owner]

            def body(s, carry):
                x = tok[s, :, tok_columns(i)]
                y = jnp.dot(x, w, preferred_element_type=F32)
                if i > 0:
                    y = acc[part, s] + y
                acc[part, s] = y
                return carry

            lax.fori_loop(0, seqs, body, 0)

    def close(i, source):
        owner = owner_at(order[i])
        where = pl.ds(pl.multiple_of(source * pos, pos), pos)
        for part in range(2):
            for s in range(seqs):
                y = jnp.dot(
                    tok[s, where, tok_columns(i)], wts[part, owner], preferred_element_type=F32
                )
                kv[part, s, where, :] = (acc[part, s, where, :] + y).astype(BF16)

    def pair_ready(hop):
        for direction in range(2):
            for sub in range(SUBS):
                if used(direction, hop, sub):
                    pair_copy(direction, hop, sub, partner).wait_recv()

    def steps_of_hop(hop):
        if hop == 0:
            return [0]
        first = 1 + 2 * (hop - 1)
        return [first, first + 1] if hop < hops else [first]

    def compute_hop(hop):
        if hop > 0:
            pair_ready(hop)
        if chunked:
            for i in steps_of_hop(hop):
                if i < len(order) - 1:
                    tokens_ready(i)
                    multiply(i)
                else:
                    close(i, tp)
                    tokens_ready(i)
                    for p in tp_peers:
                        close(i, p)

    for hop in range(1, hops + 1):
        for sub in range(SUBS):
            for direction in range(2):
                if not used(direction, hop, sub):
                    continue
                got(direction, hop, sub).wait_recv()
                if hop < hops and used(direction, hop + 1, sub):
                    launch(sent(direction, hop + 1, sub))
                launch(pair_copy(direction, hop, sub, gr))
        compute_hop(hop - 1)
    compute_hop(hops)

    if not chunked:
        tokens_ready(0)
        tile = pos
        for part in range(2):
            w = wts[part].reshape(width, cols)

            def body(j, carry):
                s, r = j // (span // tile), lax.rem(j, span // tile)
                where = pl.ds(pl.multiple_of(r * tile, tile), tile)
                y = jnp.dot(tok[s, where, :], w, preferred_element_type=F32)
                kv[part, s, where, :] = y.astype(BF16)
                return carry

            lax.fori_loop(0, seqs * (span // tile), body, 0)

    for k in range(tp_count - 1):
        bias_move(k, lax.rem(tp + tp_count - k - 1, tp_count), tp).wait_recv()
    bias[tp] = bias_all[:, tp]

    row_id = lax.broadcasted_iota(jnp.int32, (rows_h, cols), 0)
    col_id = lax.broadcasted_iota(jnp.int32, (rows_h, cols), 1)
    own = row_id == col_id // head_dim
    q = query[:, pl.ds(col_start, cols)].astype(F32)
    total_heads = offset.shape[1]
    pick = lax.broadcasted_iota(jnp.int32, (rows_h, total_heads), 1) == (
        lax.broadcasted_iota(jnp.int32, (rows_h, total_heads), 0) + tp * heads
    )
    offset_col = jnp.sum(jnp.where(pick, offset[...], 0.0), axis=1, keepdims=True)
    logits = []
    for s in range(seqs):
        q_rows = jnp.where(own, q[s : s + 1], 0.0).astype(BF16)
        b = jnp.concatenate([bias[t, s] for t in range(tp_count)], axis=1)
        bias_out[s] = b
        b = b.astype(F32)
        if rows_h > heads:
            b = jnp.concatenate([b, jnp.zeros((rows_h - heads, span), F32)], axis=0)
        logits.append(
            lax.dot_general(
                q_rows, kv[0, s], (((1,), (1,)), ((), ())), preferred_element_type=F32
            )
            * (head_dim**-0.5)
            + offset_col
            + b
        )
    logits = jnp.concatenate(logits, axis=0)
    soft = jnp.log1p(jnp.exp(-jnp.abs(logits)))
    fading = -jnp.maximum(logits, 0.0) - soft
    taking = jnp.minimum(logits, 0.0) - soft
    high = fading.astype(BF16)
    rest = fading - high.astype(F32)
    mid = rest.astype(BF16)
    low = (rest - mid.astype(F32)).astype(BF16)
    later = (
        lax.broadcasted_iota(jnp.int32, (span, span), 0)
        > lax.broadcasted_iota(jnp.int32, (span, span), 1)
    ).astype(F32).astype(BF16)
    sums = jnp.dot(
        jnp.concatenate([high, mid, low], axis=0), later, preferred_element_type=F32
    )
    m = seqs * rows_h
    within = sums[:m] + sums[m : 2 * m] + sums[2 * m :]
    weights = jnp.exp(taking + within).astype(BF16)
    totals = jnp.sum(fading, axis=1, keepdims=True)
    for s in range(seqs):
        at = slice(s * rows_h, (s + 1) * rows_h)
        partial = jnp.dot(weights[at], kv[1, s], preferred_element_type=F32)
        packed[me, s : s + 1] = jnp.sum(jnp.where(own, partial, 0.0), axis=0, keepdims=True)
        packed[me, seqs + s : seqs + s + 1] = jnp.sum(
            jnp.where(own, totals[at], 0.0), axis=0, keepdims=True
        )

    def mix_move(k, source):
        return pltpu.make_async_remote_copy(
            src_ref=packed.at[source], dst_ref=packed.at[source],
            send_sem=mix_send.at[k - 1], recv_sem=mix_recv.at[k - 1],
            device_id={"sp": lax.rem(me + k, n)}, device_id_type=MESH,
        )

    for k in range(1, n):
        launch(mix_move(k, me))
    for k in range(1, n):
        mix_move(k, lax.rem(me + n - k, n)).wait_recv()
    for c in sent_list:
        c.wait_send()


def finish(n, head_dim, kv, bias, packed, key_out, value_out, bias_out, reading_out, sems):
    moves = [
        pltpu.make_async_copy(kv.at[0], key_out, sems.at[0]),
        pltpu.make_async_copy(kv.at[1], value_out, sems.at[1]),
        pltpu.make_async_copy(bias, bias_out, sems.at[2]),
    ]
    for c in moves:
        c.start()
    seqs, cols = reading_out.shape
    rows_h = max(8, cols // head_dim)
    row_id = lax.broadcasted_iota(jnp.int32, (rows_h, cols), 0)
    col_id = lax.broadcasted_iota(jnp.int32, (rows_h, cols), 1)
    own = row_id == col_id // head_dim
    mixture = jnp.zeros((seqs, cols), F32)
    carry = jnp.zeros((seqs, cols), F32)
    for at in range(n - 1, -1, -1):
        mixture = mixture + jnp.exp(carry) * packed[at, :seqs]
        carry = carry + packed[at, seqs:]
    for s in range(seqs):
        x = mixture[s : s + 1]
        mean = jnp.sum(jnp.where(own, x * x, 0.0), axis=1, keepdims=True) / head_dim
        scale = jnp.sum(jnp.where(own, lax.rsqrt(mean + 1e-06), 0.0), axis=0, keepdims=True)
        reading_out[s : s + 1] = x * scale
    for c in moves:
        c.wait()


def per_device(tokens, key_weight, value_weight, queries, head_offset, key_bias):
    n, tp_count = lax.axis_size("sp"), lax.axis_size("tp")
    assert n % 2 == 0 and lax.axis_size("gr") == 2
    seqs, pos, width = tokens.shape
    rows, kv_width = key_weight.shape
    head_count = head_offset.shape[0]
    head_dim = kv_width // head_count
    cols = kv_width // tp_count
    heads = head_count // tp_count
    rows_h = max(8, heads)
    span = tp_count * pos
    hops = n // 2
    bias_rows = jnp.transpose(key_bias, (0, 2, 1)).reshape(seqs, tp_count, heads, pos)
    dims = (n, tp_count, seqs, pos, width, rows, cols, heads, head_dim, rows_h)
    peers = max(tp_count - 1, 1)
    chunks = n if (width // n) % 128 == 0 else 1
    dma = pltpu.SemaphoreType.DMA
    kv, bias_held, packed = pl.pallas_call(
        functools.partial(kernel, dims),
        out_shape=(
            jax.ShapeDtypeStruct((2, seqs, span, cols), BF16),
            jax.ShapeDtypeStruct((seqs, heads, span), BF16),
            jax.ShapeDtypeStruct((n, 2 * seqs, cols), F32),
        ),
        in_specs=[pl.BlockSpec(memory_space=pltpu.HBM)] * 6,
        out_specs=[pl.BlockSpec(memory_space=pltpu.VMEM)] * 3,
        scratch_shapes=[
            pltpu.VMEM((seqs, span, width), BF16),
            pltpu.VMEM((2, n, rows, cols), BF16),
            pltpu.VMEM((2, seqs, span, cols), F32),
            pltpu.VMEM((tp_count, seqs, heads, pos), BF16),
            pltpu.VMEM(queries.shape, BF16),
            pltpu.VMEM((1, head_count), F32),
            pltpu.VMEM((seqs, tp_count, heads, pos), BF16),
            dma((6,)),
            dma((2, hops, SUBS)),
            dma((2, hops, SUBS)),
            dma((2, hops, SUBS)),
            dma((2, hops, SUBS)),
            dma((chunks, peers)),
            dma((chunks, peers)),
            dma((peers,)),
            dma((peers,)),
            dma((n - 1,)),
            dma((n - 1,)),
        ],
        compiler_params=pltpu.CompilerParams(
            collective_id=0, has_side_effects=True, vmem_limit_bytes=36 * 2**20
        ),
        name="prefill",
    )(*(pltpu.with_memory_space_constraint(a, pltpu.HBM) for a in (tokens, key_weight, value_weight, queries, head_offset.reshape(1, head_count), bias_rows)))
    key_cache, value_cache, bias_cache, reading = pl.pallas_call(
        functools.partial(finish, n, head_dim),
        out_shape=(
            jax.ShapeDtypeStruct((seqs, span, cols), BF16),
            jax.ShapeDtypeStruct((seqs, span, cols), BF16),
            jax.ShapeDtypeStruct((seqs, heads, span), BF16),
            jax.ShapeDtypeStruct((seqs, cols), F32),
        ),
        in_specs=[
            pl.BlockSpec(memory_space=pl.ANY),
            pl.BlockSpec(memory_space=pl.ANY),
            pl.BlockSpec(memory_space=pltpu.VMEM),
        ],
        out_specs=[
            pl.BlockSpec(memory_space=pl.ANY),
            pl.BlockSpec(memory_space=pl.ANY),
            pl.BlockSpec(memory_space=pl.ANY),
            pl.BlockSpec(memory_space=pltpu.VMEM),
        ],
        scratch_shapes=[dma((3,))],
        compiler_params=pltpu.CompilerParams(vmem_limit_bytes=4 * 2**20),
        name="finish",
    )(kv, bias_held, packed)
    return key_cache, value_cache, jnp.transpose(bias_cache, (0, 2, 1)), reading


def solution(mesh):
    in_specs = (
        P("gr", ("sp", "tp"), None),
        P("sp", None),
        P("sp", None),
        P("gr", None),
        P(),
        P("gr", ("sp", "tp"), None),
    )
    out_specs = (P("gr", "sp", "tp"), P("gr", "sp", "tp"), P("gr", "sp", "tp"), P("gr", "tp"))
    return jax.shard_map(
        per_device, mesh=mesh, in_specs=in_specs, out_specs=out_specs, check_vma=False
    )
```
